256 devices in a mesh: grp: 2 (over z), ep: 64 (over y, x), tp: 2 (over core).
Axes of the slice: x: 8, y: 8, z: 2, core: 2. Of those that a mesh axis runs over, the one named last changes fastest.
The devices are a block of a 8x8x16 slice.
Arguments:
- tokens: bfloat16 [32768, 2048], P(('grp', 'ep', 'tp')), parts along dimension 0, may hold values from -6 to 6
- norm_gain: float32 [2048], replicated, may hold values from 0.1 to 1.9
- expert_ids: int32 [32768, 2], P(('grp', 'ep', 'tp')), parts along dimension 0, may hold values from 0 to 63, as said below
- gate_weights: float32 [32768, 2], P(('grp', 'ep', 'tp')), parts along dimension 0, may hold values from 0.1 to 1
- w_gate: bfloat16 [64, 2048, 512], P('ep', None, 'tp'), may hold values from -0.125 to 0.125
- w_up: bfloat16 [64, 2048, 512], P('ep', None, 'tp'), may hold values from -0.125 to 0.125
- w_down: bfloat16 [64, 512, 2048], P('ep', 'tp'), may hold values from -0.25 to 0.25
Outputs:
- mixed: bfloat16 [32768, 2048], P(('grp', 'ep', 'tp')), parts along dimension 0
The draws below stay inside these ranges and needn't reach their ends.
There are 2 independent parts, one for each index of `grp`. The reference program is written for one: setup_inputs(seed, part) draws one part's arguments, and reference() takes and returns one part's arrays. A program takes and returns all parts, laid end to end along the dimension named above; an argument that names none is the same for every part. Nothing has to cross between parts.
Inputs may be any that keep to these rules, and one draw needn't show every extreme that they name: `expert_ids`: the 2 experts of a token are different and lie in one group of 16 consecutive experts. Among the rows of one device (aligned blocks of 128 rows) no expert is named more than 8 times, and in every such block some expert is named exactly 8 times.
All inputs are finite; a program needn't handle non-finite values.
Results may differ from the reference program's by a relative error of at most 0.0078.
Values may be sent and summed in bfloat16 or wider, within the bound.
A program may use at most 64 MiB of HBM per device.

```python
import math
import jax
import jax.numpy as jnp
from jax import lax

D = 2048
FF = 512
N_GROUPS = 4
TOP_K = 2
TOK_DEV = 128
EXPERTS = 64
TOKENS = 16384
N_TP = 2


def draw_expert_ids(key, part):
    n_blocks = TOKENS // TOK_DEV
    per_group = EXPERTS // N_GROUPS
    half_rows = TOK_DEV // 2
    keys = jax.random.split(jax.random.fold_in(key, 17), 8)
    favored = jax.random.randint(keys[0], (), 0, N_GROUPS)
    coin = jax.random.randint(keys[1], (n_blocks,), 0, 2)
    other = jax.random.randint(keys[2], (n_blocks,), 0, N_GROUPS)
    busiest = jnp.where(coin == 1, favored, other)
    first_size = jax.random.randint(keys[3], (n_blocks,), 0, half_rows + 1)
    second_size = jax.random.randint(keys[4], (n_blocks,), 0, half_rows + 1) % (half_rows - first_size + 1)
    third_size = half_rows - first_size - second_size
    sizes = jnp.stack([jnp.full((n_blocks,), half_rows, jnp.int32), first_size, second_size, third_size], axis=1)
    ends = jnp.cumsum(sizes, axis=1)
    begins = ends - sizes
    position = jnp.arange(TOK_DEV, dtype=jnp.int32)
    rank = jnp.sum((position[None, :, None] >= ends[:, None, :]).astype(jnp.int32), axis=2)
    rank = jnp.minimum(rank, N_GROUPS - 1)
    inner = position[None, :] - jnp.take_along_axis(begins, rank, axis=1)
    group = (busiest[:, None] + rank) % N_GROUPS
    offset = jax.random.randint(keys[5], (n_blocks, 1), 0, per_group)
    stride = jax.random.randint(keys[6], (n_blocks, 1), 1, (per_group - 1) // (TOP_K - 1) + 1)
    choice_index = jnp.arange(TOP_K, dtype=jnp.int32)
    within = (offset[:, :, None] + inner[:, :, None] + choice_index[None, None, :] * stride[:, :, None]) % per_group
    by_position = group[:, :, None] * per_group + within
    orders = jax.vmap(lambda sub: jax.random.permutation(sub, TOK_DEV))(jax.random.split(keys[7], n_blocks))
    inverse = jnp.argsort(orders, axis=1, stable=True)
    by_token = jnp.take_along_axis(by_position, inverse[:, :, None], axis=1)
    return by_token.reshape(TOKENS, TOP_K).astype(jnp.int32)


def shard_levels(stream_key, dims, pieces, least, top_value):
    def one(dim, blocks):
        heights = jax.random.uniform(jax.random.fold_in(jax.random.fold_in(stream_key, 6), dim), (blocks,), jnp.float32, least / len(pieces), top_value / len(pieces))
        return jnp.repeat(jnp.exp(heights), dims[dim] // blocks).reshape((-1,) + (1,) * (len(dims) - dim - 1))

    gain = one(*pieces[0])
    for cut in pieces[1:]:
        gain = gain * one(*cut)
    return gain


def noise(own_key, shape, spread, most, cuts=(), kind=jnp.bfloat16):
    gain = shard_levels(own_key, shape, cuts, -0.22, 0.18) if cuts else 1.0
    result = jax.random.normal(own_key, shape, jnp.float32) * spread * gain
    return jnp.minimum(jnp.maximum(result, -most), most).astype(kind)


def setup_inputs(seed: int = 0, part: int = 0) -> dict:
    key_of = jax.random.split(jax.random.key(seed), 8)
    part_splits = jax.random.split(jax.random.fold_in(key_of[7], part), 8)
    return {
        "tokens": noise(part_splits[0], (TOKENS, D), 1.0, 6.0, ((0, 128),)),
        "norm_gain": jnp.clip(1.0 + 0.18 * jax.random.normal(key_of[1], (D,), jnp.float32), 0.1, 1.9),
        "expert_ids": draw_expert_ids(jax.random.fold_in(jax.random.fold_in(key_of[7], part), 71), part),
        "gate_weights": jnp.clip(jnp.exp(math.log(1.0) - 2.3025851 * jax.random.uniform(part_splits[3], (TOKENS, TOP_K), jnp.float32) ** shard_levels(part_splits[3], (TOKENS, TOP_K), ((0, 128),), -0.2, 0.2)), 0.1, 1.0),
        "w_gate": noise(key_of[4], (EXPERTS, D, FF), D ** -0.5, 0.125, ((0, 64), (2, 2))),
        "w_up": noise(key_of[5], (EXPERTS, D, FF), D ** -0.5, 0.125, ((0, 64), (2, 2))),
        "w_down": noise(key_of[6], (EXPERTS, FF, D), FF ** -0.5, 0.25, ((0, 64), (1, 2))),
    }


def reference(tokens, norm_gain, expert_ids, gate_weights, w_gate, w_up, w_down):
    values = tokens.astype(jnp.float32)
    normed = (values * lax.rsqrt(lax.optimization_barrier(jnp.mean(values * values, axis=-1, keepdims=True)) + 1e-06) * norm_gain).astype(jnp.bfloat16)
    n_tok = normed.shape[0]
    model_width = normed.shape[1]
    top_count = expert_ids.shape[1]
    total = n_tok * top_count
    block_rows = 128
    n_blocks = (total + EXPERTS * (block_rows - 1) + block_rows - 1) // block_rows
    flat_e = expert_ids.reshape(-1).astype(jnp.int32)
    flat_tok = (jnp.arange(total, dtype=jnp.int32) // top_count).astype(jnp.int32)
    sorted_order = jnp.argsort(flat_e, stable=True).astype(jnp.int32)
    sorted_e = flat_e[sorted_order]
    expert_counts = jnp.bincount(flat_e, length=EXPERTS).astype(jnp.int32)
    starts = (jnp.cumsum(expert_counts) - expert_counts).astype(jnp.int32)
    padded_counts = ((expert_counts + block_rows - 1) // block_rows * block_rows).astype(jnp.int32)
    padded_ends = jnp.cumsum(padded_counts).astype(jnp.int32)
    padded_starts = (padded_ends - padded_counts).astype(jnp.int32)
    dest_index = (padded_starts[sorted_e] + jnp.arange(total, dtype=jnp.int32) - starts[sorted_e]).astype(jnp.int32)
    rows_tok = jnp.full((n_blocks * block_rows,), n_tok, jnp.int32).at[dest_index].set(flat_tok[sorted_order])
    rows_gate = jnp.zeros((n_blocks * block_rows,), jnp.float32).at[dest_index].set(gate_weights.reshape(-1)[sorted_order])
    block_e = jnp.minimum(jnp.searchsorted(padded_ends, jnp.arange(n_blocks, dtype=jnp.int32) * block_rows, side='right'), EXPERTS - 1).astype(jnp.int32)
    x_pad = jnp.concatenate([normed, jnp.zeros((1, model_width), normed.dtype)], axis=0)
    hidden_block = FF // N_TP

    def run_block(inputs):
        expert, toks = inputs
        rows_in = x_pad[toks]
        gate_act = jnp.dot(rows_in, w_gate[expert], preferred_element_type=jnp.float32)
        up_act = jnp.dot(rows_in, w_up[expert], preferred_element_type=jnp.float32)
        hidden = (jax.nn.silu(gate_act) * up_act).astype(jnp.bfloat16)
        down = w_down[expert]
        acc = jnp.zeros((rows_in.shape[0], model_width), jnp.float32)
        for index in range(N_TP):
            partial_value = jnp.dot(hidden[:, index * hidden_block:(index + 1) * hidden_block], down[index * hidden_block:(index + 1) * hidden_block], preferred_element_type=jnp.float32)
            rounded = lax.optimization_barrier(partial_value.astype(jnp.bfloat16))
            acc = acc + rounded.astype(jnp.float32)
        return acc.astype(jnp.bfloat16)
    outputs = lax.map(run_block, (block_e, rows_tok.reshape(n_blocks, block_rows)))
    mixed = jnp.zeros((n_tok + 1, model_width), jnp.float32).at[rows_tok].add(outputs.reshape(-1, model_width).astype(jnp.float32) * rows_gate[:, None])
    return mixed[:n_tok].astype(jnp.bfloat16)
```

```python
import functools
import math

import jax
import jax.numpy as jnp
from jax import lax
from jax.experimental import pallas as pl
from jax.experimental.pallas import tpu as pltpu
from jax.sharding import PartitionSpec as P

N_GROUPS = 4
BLOCKS = 4
MESH = pl.DeviceIdType.MESH
BF16 = jnp.bfloat16
F32 = jnp.float32


def kernel(
    n_ep,
    side,
    cap,
    tokens_ref,
    gain_ref,
    ids_ref,
    gates_ref,
    wg_hbm,
    wu_hbm,
    wd_hbm,
    out_ref,
    normed,
    pick0,
    pick1,
    buckets,
    recv,
    outs,
    results,
    wg,
    wu,
    wd,
    acc,
    local_sem,
    wsend_sem,
    wrecv_sem,
    dsend_sem,
    drecv_sem,
    csend_sem,
    crecv_sem,
):
    ep = lax.axis_index("ep")
    tp = lax.axis_index("tp")
    my, mx = ep // side, lax.rem(ep, side)
    per_block = n_ep // BLOCKS
    rows = per_block * cap
    n_tok = tokens_ref.shape[0]
    n_slots = n_ep * cap

    def offset(o):
        block, j = o // per_block, lax.rem(o, per_block)
        dx = j // 2
        dy = lax.rem(block + side - dx, BLOCKS) + BLOCKS * lax.rem(j, 2)
        return dy, dx

    def ahead(o):
        dy, dx = offset(o)
        return lax.rem(my + dy, side) * side + lax.rem(mx + dx, side)

    def behind(o):
        dy, dx = offset(o)
        return lax.rem(my + side - dy, side) * side + lax.rem(mx + side - dx, side)

    barrier = pltpu.get_barrier_semaphore()

    @pl.loop(1, n_ep)
    def _(i):
        pl.semaphore_signal(
            barrier, inc=1, device_id={"ep": lax.rem(ep + i, n_ep)}, device_id_type=MESH
        )

    pl.semaphore_signal(barrier, inc=1, device_id={"tp": 1 - tp}, device_id_type=MESH)

    local = [
        pltpu.make_async_copy(src.at[0], dst.at[tp], local_sem.at[i])
        for i, (src, dst) in enumerate(((wg_hbm, wg), (wu_hbm, wu), (wd_hbm, wd)))
    ]
    for copy in local:
        copy.start()

    values = tokens_ref[...].astype(F32)
    scale = lax.rsqrt(jnp.mean(values * values, axis=-1, keepdims=True) + 1e-06)
    normed[...] = (values * scale * gain_ref[...]).astype(BF16)

    ids = ids_ref[...]
    experts = [ids[:, k : k + 1] for k in range(ids.shape[1])]
    lanes = lax.broadcasted_iota(jnp.int32, (n_tok, n_ep), 1)
    hots = [(e == lanes).astype(F32) for e in experts]
    earlier = (
        lax.broadcasted_iota(jnp.int32, (n_tok, n_tok), 0)
        > lax.broadcasted_iota(jnp.int32, (n_tok, n_tok), 1)
    ).astype(BF16)
    before = jnp.dot(earlier, sum(hots).astype(BF16), preferred_element_type=F32)
    slots = lax.broadcasted_iota(jnp.int32, (n_tok, n_slots), 1)
    for e, hot, pick in zip(experts, hots, (pick0, pick1)):
        place = jnp.sum(before * hot, axis=1, keepdims=True).astype(jnp.int32)
        dy = (e // side - my + side) % side
        dx = (e % side - mx + side) % side
        order = (dx + dy) % BLOCKS * per_block + dx * 2 + dy // BLOCKS
        hot_slot = (order * cap + place == slots).astype(BF16)
        for b in range(BLOCKS):
            pick[b] = hot_slot[:, b * rows : (b + 1) * rows]

    def bucket(b):
        block = pl.ds(b * rows, rows)
        buckets[block, :] = lax.dot_general(
            pick0[b] + pick1[b], normed[...], (((0,), (0,)), ((), ())), preferred_element_type=F32
        ).astype(BF16)

    def part(o):
        return pl.ds(pl.multiple_of(o * cap, cap), cap)

    def dispatch(o):
        return pltpu.make_async_remote_copy(
            src_ref=buckets.at[part(o)],
            dst_ref=recv.at[part(o)],
            send_sem=dsend_sem.at[o],
            recv_sem=drecv_sem.at[o],
            device_id={"ep": ahead(o)},
            device_id_type=MESH,
        )

    def giveback(o):
        return pltpu.make_async_remote_copy(
            src_ref=outs.at[part(o)],
            dst_ref=results.at[part(o)],
            send_sem=csend_sem.at[o],
            recv_sem=crecv_sem.at[o],
            device_id={"ep": behind(o)},
            device_id_type=MESH,
        )

    def shuffled(b, j):
        return b * per_block + lax.rem(j * 5 + mx * 3 + my * 7, per_block)

    def send_block(make, b):
        @pl.loop(0, per_block)
        def _(j):
            o = shuffled(b, j)

            @pl.when(o != 0)
            def _():
                make(o).start()

    def await_block(make, b):
        @pl.loop(0, per_block)
        def _(j):
            o = b * per_block + j

            @pl.when(o != 0)
            def _():
                make(o).wait_recv()

    bucket(0)
    pl.semaphore_wait(barrier, n_ep)
    send_block(dispatch, 0)
    for copy in local:
        copy.wait()
    swaps = [
        pltpu.make_async_remote_copy(
            src_ref=ref.at[tp],
            dst_ref=ref.at[tp],
            send_sem=wsend_sem.at[i],
            recv_sem=wrecv_sem.at[i],
            device_id={"tp": 1 - tp},
            device_id_type=MESH,
        )
        for i, ref in enumerate((wg, wu, wd))
    ]
    for swap in swaps:
        swap.start()

    @pl.loop(1, BLOCKS)
    def _(b):
        bucket(b)
        send_block(dispatch, b)

    recv[:cap, :] = buckets[:cap, :]
    for swap in swaps:
        swap.wait()

    @pl.loop(0, BLOCKS)
    def _(b):
        await_block(dispatch, b)
        block = pl.ds(b * rows, rows)
        taken = recv[block, :]
        total = None
        for j in range(wg.shape[0]):
            gate_act = jnp.dot(taken, wg[j], preferred_element_type=F32)
            up_act = jnp.dot(taken, wu[j], preferred_element_type=F32)
            hidden = (gate_act / (1.0 + jnp.exp(-gate_act)) * up_act).astype(BF16)
            partial = jnp.dot(hidden, wd[j], preferred_element_type=F32).astype(BF16).astype(F32)
            total = partial if total is None else total + partial
        outs[block, :] = total.astype(BF16)
        send_block(giveback, b)

    results[:cap, :] = outs[:cap, :]
    gates = gates_ref[...]
    acc[...] = jnp.zeros_like(acc)

    @pl.loop(0, BLOCKS)
    def _(b):
        await_block(giveback, b)
        back = results[pl.ds(b * rows, rows), :]
        acc[...] += (
            jnp.dot(pick0[b], back, preferred_element_type=F32) * gates[:, 0:1]
            + jnp.dot(pick1[b], back, preferred_element_type=F32) * gates[:, 1:2]
        )

    out_ref[...] = acc[...].astype(BF16)

    @pl.loop(1, n_ep)
    def _(o):
        dispatch(o).wait_send()
        giveback(o).wait_send()


def shards(n_ep, n_tp, tokens, norm_gain, expert_ids, gate_weights, w_gate, w_up, w_down):
    n_tok, width = tokens.shape
    top_count = expert_ids.shape[1]
    n_exp = w_gate.shape[0] * n_ep
    side = math.isqrt(n_ep)
    cap = top_count * (n_tok // 2) // (n_exp // N_GROUPS)
    n_slots = n_exp * cap
    rows = n_slots // BLOCKS
    hidden = w_gate.shape[2]
    vmem = pl.BlockSpec(memory_space=pltpu.VMEM)
    anywhere = pl.BlockSpec(memory_space=pl.ANY)
    dma = pltpu.SemaphoreType.DMA
    return pl.pallas_call(
        functools.partial(kernel, n_ep, side, cap),
        out_shape=jax.ShapeDtypeStruct((n_tok, width), BF16),
        in_specs=[vmem] * 4 + [anywhere] * 3,
        out_specs=vmem,
        scratch_shapes=[
            pltpu.VMEM((n_tok, width), BF16),
            pltpu.VMEM((BLOCKS, n_tok, rows), BF16),
            pltpu.VMEM((BLOCKS, n_tok, rows), BF16),
            pltpu.VMEM((n_slots, width), BF16),
            pltpu.VMEM((n_slots, width), BF16),
            pltpu.VMEM((n_slots, width), BF16),
            pltpu.VMEM((n_slots, width), BF16),
            pltpu.VMEM((n_tp, width, hidden), BF16),
            pltpu.VMEM((n_tp, width, hidden), BF16),
            pltpu.VMEM((n_tp, hidden, width), BF16),
            pltpu.VMEM((n_tok, width), F32),
            dma((3,)),
            dma((3,)),
            dma((3,)),
            dma((n_ep,)),
            dma((n_ep,)),
            dma((n_ep,)),
            dma((n_ep,)),
        ],
        compiler_params=pltpu.CompilerParams(
            collective_id=0, has_side_effects=True, vmem_limit_bytes=60 * 1024 * 1024
        ),
    )(tokens, norm_gain.reshape(1, width), expert_ids, gate_weights, w_gate, w_up, w_down)


def solution(mesh):
    placed = (
        P(("grp", "ep", "tp"), None),
        P(),
        P(("grp", "ep", "tp"), None),
        P(("grp", "ep", "tp"), None),
        P("ep", None, "tp"),
        P("ep", None, "tp"),
        P("ep", "tp", None),
    )
    return jax.shard_map(
        functools.partial(shards, mesh.shape["ep"], mesh.shape["tp"]),
        mesh=mesh,
        in_specs=placed,
        out_specs=P(("grp", "ep", "tp"), None),
        check_vma=False,
    )
```

```python
import functools
import math

import jax
import jax.numpy as jnp
from jax import lax
from jax.experimental import pallas as pl
from jax.experimental.pallas import tpu as pltpu
from jax.sharding import PartitionSpec as P

N_GROUPS = 4
MESH = pl.DeviceIdType.MESH
BF16 = jnp.bfloat16
F32 = jnp.float32


def kernel(
    side,
    cap,
    cut,
    tokens_ref,
    gain_ref,
    ids_ref,
    gates_ref,
    wg_hbm,
    wu_hbm,
    wd_hbm,
    out_ref,
    pick,
    weigh_hi,
    weigh_lo,
    bkt_a,
    bkt_b,
    mid_a,
    mid_b,
    recv_a,
    recv_b,
    outs_a,
    outs_b,
    back_a,
    back_b,
    res_a,
    res_b,
    wg,
    wu,
    wd,
    acc,
    local_sem,
    swap_sem,
    line_sem,
    turn_a_sem,
    turn_b_sem,
):
    n_ep = side * side
    half = side // 2
    pairs = half
    ep = lax.axis_index("ep")
    tp = lax.axis_index("tp")
    my, mx = ep // side, lax.rem(ep, side)
    n_tok = tokens_ref.shape[0]
    rows = 2 * side * cap

    def shift(p):
        k = p // 2
        return jnp.where(p % 2 == 0, k, jnp.where(k == 0, half, side - k))

    def in_row(p, sign):
        return my * side + lax.rem(mx + side + sign * shift(p), side)

    def in_column(q, sign):
        return lax.rem(my + side + sign * shift(q), side) * side + mx

    def remote(src, dst, sems, at, target):
        return pltpu.make_async_remote_copy(
            src_ref=src,
            dst_ref=dst,
            send_sem=sems.at[(0, *at)],
            recv_sem=sems.at[(1, *at)],
            device_id={"ep": target},
            device_id_type=MESH,
        )

    def out1_a(p):
        return remote(bkt_a.at[p], mid_a.at[p], line_sem, (0, p), in_row(p, 1))

    def out1_b(q):
        return remote(bkt_b.at[q], mid_b.at[q], line_sem, (1, q), in_column(q, 1))

    def out2_a(c, q):
        two = pl.ds(2 * c, 2)
        return remote(mid_a.at[two, q], recv_a.at[two, q], turn_a_sem, (0, c, q), in_column(q, 1))

    def out2_b(h, p):
        some = pl.ds(h * half, half)
        return remote(mid_b.at[some, p], recv_b.at[p, some], turn_b_sem, (h, p), in_row(p, 1))

    def in1_a(c, q):
        two = pl.ds(2 * c, 2)
        return remote(outs_a.at[two, q], back_a.at[two, q], turn_a_sem, (1, c, q), in_column(q, -1))

    def in1_b(p):
        return remote(outs_b.at[p], back_b.at[p], line_sem, (2, p), in_row(p, -1))

    def in2_a(p):
        return remote(back_a.at[p], res_a.at[p], line_sem, (3, p), in_row(p, -1))

    def in2_b(c, q):
        two = pl.ds(2 * c, 2)
        return remote(back_b.at[two, q], res_b.at[two, q], turn_a_sem, (2, c, q), in_column(q, -1))

    barrier = pltpu.get_barrier_semaphore()

    @pl.loop(1, side)
    def _(p):
        pl.semaphore_signal(barrier, inc=1, device_id={"ep": in_row(p, 1)}, device_id_type=MESH)
        pl.semaphore_signal(barrier, inc=1, device_id={"ep": in_column(p, 1)}, device_id_type=MESH)

    pl.semaphore_signal(barrier, inc=1, device_id={"tp": 1 - tp}, device_id_type=MESH)

    local = [
        pltpu.make_async_copy(src.at[0], dst.at[tp], local_sem.at[i])
        for i, (src, dst) in enumerate(((wg_hbm, wg), (wu_hbm, wu), (wd_hbm, wd)))
    ]
    for copy in local:
        copy.start()

    ids = ids_ref[...]
    gates = gates_ref[...]
    below = lax.broadcasted_iota(jnp.int32, (n_ep, n_tok), 0)
    hots = [(ids[k : k + 1] == below).astype(F32) for k in range(ids.shape[0])]
    earlier = (
        lax.broadcasted_iota(jnp.int32, (n_tok, n_tok), 0)
        < lax.broadcasted_iota(jnp.int32, (n_tok, n_tok), 1)
    ).astype(BF16)
    before = jnp.dot(sum(hots).astype(BF16), earlier, preferred_element_type=F32)

    def place(d):
        return jnp.where(d == 0, 0, jnp.where(d == half, 1, jnp.where(d < half, 2 * d, 2 * (side - d) + 1)))

    slots = []
    for k, hot in enumerate(hots):
        e = ids[k : k + 1]
        nth = jnp.sum(before * hot, axis=0, keepdims=True).astype(jnp.int32)
        q = place((e // side - my + side) % side)
        p = place((e % side - mx + side) % side)
        slots.append((p * side + q) * cap + nth)
    gates_hi = gates.astype(BF16).astype(F32)
    gates_lo = gates - gates_hi
    for c in range(pairs):
        row = lax.broadcasted_iota(jnp.int32, (rows, n_tok), 0) + c * rows
        picks = [slot == row for slot in slots]
        pick[c] = sum(x.astype(F32) for x in picks).astype(BF16)
        for weigh, g in ((weigh_hi, gates_hi), (weigh_lo, gates_lo)):
            weigh[c] = sum(jnp.where(x, g[k : k + 1], 0.0) for k, x in enumerate(picks)).astype(BF16)

    values = tokens_ref[...].astype(F32)
    scale = lax.rsqrt(jnp.mean(values * values, axis=-1, keepdims=True) + 1e-06)
    normed = (values * scale * gain_ref[...]).astype(BF16)
    for c in range(pairs):
        bucket = jnp.dot(pick[c], normed, preferred_element_type=F32).astype(BF16)
        bkt_a[pl.ds(2 * c, 2)] = bucket[:, :cut].reshape(2, side, cap, cut)
        for i in range(2):
            bkt_b[:, 2 * c + i] = bucket[i * (rows // 2) : (i + 1) * (rows // 2), cut:].reshape(side, cap, -1)

    pl.semaphore_wait(barrier, 2 * side - 1)

    @pl.loop(1, side)
    def _(p):
        out1_a(p).start()
        out1_b(p).start()

    for copy in local:
        copy.wait()
    swaps = [
        pltpu.make_async_remote_copy(
            src_ref=ref.at[tp],
            dst_ref=ref.at[tp],
            send_sem=swap_sem.at[0, i],
            recv_sem=swap_sem.at[1, i],
            device_id={"tp": 1 - tp},
            device_id_type=MESH,
        )
        for i, ref in enumerate((wg, wu, wd))
    ]
    for swap in swaps:
        swap.start()

    mid_a[0] = bkt_a[0]
    mid_b[0] = bkt_b[0]

    def turn_b(h):
        @pl.loop(max(1, h * half), (h + 1) * half)
        def _(q):
            out1_b(q).wait_recv()

        @pl.loop(1, side)
        def _(p):
            out2_b(h, p).start()

    def turn_a(c):
        if c:
            out1_a(2 * c).wait_recv()
        out1_a(2 * c + 1).wait_recv()

        @pl.loop(1, side)
        def _(q):
            out2_a(c, q).start()

    for c in range(pairs):
        turn_a(c)
        if c % 2:
            turn_b(c // 2)

    recv_a[:, 0] = mid_a[:, 0]
    recv_b[0] = mid_b[:, 0]
    for swap in swaps:
        swap.wait()

    @pl.loop(0, pairs)
    def _(c):
        @pl.loop(1, side)
        def _(q):
            out2_a(c, q).wait_recv()

        @pl.when(c > 0)
        def _():
            for h in range(2):
                out2_b(h, 2 * c).wait_recv()

        for h in range(2):
            out2_b(h, 2 * c + 1).wait_recv()

        two = pl.ds(2 * c, 2)
        taken_a = recv_a[two].reshape(rows, -1)
        taken_b = recv_b[two].reshape(rows, -1)
        total = None
        for j in range(wg.shape[0]):
            gate_act, up_act = (
                jnp.dot(taken_a, w[j, :cut], preferred_element_type=F32)
                + jnp.dot(taken_b, w[j, cut:], preferred_element_type=F32)
                for w in (wg, wu)
            )
            hidden = (gate_act / (1.0 + jnp.exp(-gate_act)) * up_act).astype(BF16)
            partial = jnp.dot(hidden, wd[j], preferred_element_type=F32).astype(BF16).astype(F32)
            total = partial if total is None else total + partial
        total = total.astype(BF16)
        outs_a[two] = total[:, :cut].reshape(2, side, cap, cut)
        outs_b[two] = total[:, cut:].reshape(2, side, cap, -1)

        @pl.loop(1, side)
        def _(q):
            in1_a(c, q).start()

        @pl.when(c > 0)
        def _():
            in1_b(2 * c).start()

        in1_b(2 * c + 1).start()

    back_a[:, 0] = outs_a[:, 0]
    back_b[0] = outs_b[0]

    for c in range(pairs):
        if c:
            in1_b(2 * c).wait_recv()
        in1_b(2 * c + 1).wait_recv()

        @pl.loop(1, side)
        def _(q):
            in2_b(c, q).start()
            in1_a(c, q).wait_recv()

        if c:
            in2_a(2 * c).start()
        in2_a(2 * c + 1).start()

    res_a[0] = back_a[0]
    res_b[:, 0] = back_b[:, 0]

    for c in range(pairs):
        if c:
            in2_a(2 * c).wait_recv()
        in2_a(2 * c + 1).wait_recv()

        @pl.loop(1, side)
        def _(q):
            in2_b(c, q).wait_recv()

        two = pl.ds(2 * c, 2)
        for res, span in ((res_a, pl.ds(0, cut)), (res_b, pl.ds(cut, tokens_ref.shape[1] - cut))):
            value = res[two].reshape(rows, -1)
            got = sum(
                lax.dot_general(w[c], value, (((0,), (0,)), ((), ())), preferred_element_type=F32)
                for w in (weigh_hi, weigh_lo)
            )
            if c:
                got = got + acc[:, span]
            if c < pairs - 1:
                acc[:, span] = got
            else:
                out_ref[:, span] = got.astype(out_ref.dtype)

    @pl.loop(1, side)
    def _(p):
        for make in (out1_a, out1_b, in1_b, in2_a):
            make(p).wait_send()
        for h in range(2):
            out2_b(h, p).wait_send()
        for c in range(pairs):
            out2_a(c, p).wait_send()
            in1_a(c, p).wait_send()
            in2_b(c, p).wait_send()


def shards(n_ep, n_tp, tokens, norm_gain, expert_ids, gate_weights, w_gate, w_up, w_down):
    n_tok, width = tokens.shape
    top_count = expert_ids.shape[1]
    n_exp = w_gate.shape[0] * n_ep
    side = math.isqrt(n_ep)
    cap = top_count * (n_tok // 2) // (n_exp // N_GROUPS)
    cut = width // 2
    rows = 2 * side * cap
    hidden = w_gate.shape[2]
    vmem = pl.BlockSpec(memory_space=pltpu.VMEM)
    anywhere = pl.BlockSpec(memory_space=pl.ANY)
    dma = pltpu.SemaphoreType.DMA
    part_a = pltpu.VMEM((side, side, cap, cut), BF16)
    part_b = pltpu.VMEM((side, side, cap, width - cut), BF16)
    mixed = pl.pallas_call(
        functools.partial(kernel, side, cap, cut),
        out_shape=jax.ShapeDtypeStruct((n_tok, width), BF16),
        in_specs=[vmem] * 4 + [anywhere] * 3,
        out_specs=vmem,
        scratch_shapes=[
            *([pltpu.VMEM((side // 2, rows, n_tok), BF16)] * 3),
            *([part_a, part_b] * 6),
            pltpu.VMEM((n_tp, width, hidden), BF16),
            pltpu.VMEM((n_tp, width, hidden), BF16),
            pltpu.VMEM((n_tp, hidden, width), BF16),
            pltpu.VMEM((n_tok, width), F32),
            dma((3,)),
            dma((2, 3)),
            dma((2, 4, side)),
            dma((2, 3, side // 2, side)),
            dma((2, 2, side)),
        ],
        compiler_params=pltpu.CompilerParams(
            collective_id=0, has_side_effects=True, vmem_limit_bytes=60 * 1024 * 1024
        ),
    )(tokens, norm_gain.reshape(1, width), expert_ids.T, gate_weights.T, w_gate, w_up, w_down)
    return mixed


def solution(mesh):
    placed = (
        P(("grp", "ep", "tp"), None),
        P(),
        P(("grp", "ep", "tp"), None),
        P(("grp", "ep", "tp"), None),
        P("ep", None, "tp"),
        P("ep", None, "tp"),
        P("ep", "tp", None),
    )
    return jax.shard_map(
        functools.partial(shards, mesh.shape["ep"], mesh.shape["tp"]),
        mesh=mesh,
        in_specs=placed,
        out_specs=P(("grp", "ep", "tp"), None),
        check_vma=False,
    )
```

```python
import functools
import math

import jax
import jax.numpy as jnp
from jax import lax
from jax.experimental import pallas as pl
from jax.experimental.pallas import tpu as pltpu
from jax.sharding import PartitionSpec as P

N_GROUPS = 4
MESH = pl.DeviceIdType.MESH
BF16 = jnp.bfloat16
F32 = jnp.float32


def kernel(
    side,
    cap,
    cut,
    tokens_ref,
    gain_ref,
    ids_ref,
    gates_ref,
    wg_hbm,
    wu_hbm,
    wd_hbm,
    out_ref,
    info,
    infos,
    weigh,
    weigh_own,
    normed_a,
    normed_b,
    tok_a,
    tok_b,
    stage_a,
    stage_b,
    mid_a,
    mid_b,
    recv_a,
    recv_b,
    outs_a,
    outs_b,
    back_a,
    back_b,
    gath_a,
    gath_b,
    part_a,
    part_b,
    land_a,
    land_b,
    wg,
    wu,
    wd,
    local_sem,
    swap_sem,
    info_sem,
    tok_sem,
    relay_sem,
    turn_sem,
    line_sem,
    cross_sem,
    gath_sem,
    part_sem,
):
    n_ep = side * side
    half = side // 2
    pairs = half
    own, far = side - 2, side - 1
    ep = lax.axis_index("ep")
    tp = lax.axis_index("tp")
    my, mx = ep // side, lax.rem(ep, side)
    n_tok = tokens_ref.shape[0]
    line = side * cap
    rows = 2 * line
    groups = [(2 * c, 2) for c in range(pairs - 1)] + [(own, 1), (far, 1)]

    def shift(p):
        k = p // 2
        return jnp.where(k == half - 1, p % 2 * half, jnp.where(p % 2 == 0, k + 1, side - 1 - k))

    def place(d):
        near = jnp.where(d < half, 2 * (d - 1), 2 * (side - d) - 1)
        return jnp.where(d == 0, own, jnp.where(d == half, far, near))

    def at_column(d):
        return my * side + lax.rem(mx + d + side, side)

    def at_row(d):
        return lax.rem(my + d + side, side) * side + mx

    def in_row(p, sign):
        return at_column(sign * shift(p))

    def in_column(q, sign):
        return at_row(sign * shift(q))

    def others(do):
        @pl.loop(0, side - 1)
        def _(i):
            do(jnp.where(i == own, far, i))

    def remote(src, dst, sems, at, target):
        return pltpu.make_async_remote_copy(
            src_ref=src,
            dst_ref=dst,
            send_sem=sems.at[(0, *at)],
            recv_sem=sems.at[(1, *at)],
            device_id={"ep": target},
            device_id_type=MESH,
        )

    def step(axis, way, far_by):
        return (at_column, at_row)[axis](far_by * (1 - 2 * way))

    normed = (normed_a, normed_b)
    tok, stage, mid = (tok_a, tok_b), (stage_a, stage_b), (mid_a, mid_b)

    def tell(axis, way):
        return remote(info, infos.at[axis, way], info_sem, (axis, way), step(axis, way, 1))

    def give(axis, way):
        return remote(normed[axis], tok[axis].at[way], tok_sem, (axis, way), step(axis, way, 1))

    def relay(axis, way, b):
        at = (axis, way, b)
        if b < 2:
            src, dst = stage[axis].at[way, pl.ds(b * side, side)], mid[axis].at[2 + 2 * b + way]
        else:
            src = stage[axis].at[way, pl.ds(2 * side, half)]
            dst = mid[axis].at[far, pl.ds(way * half, half)]
        return remote(src, dst, relay_sem, at, step(axis, way, b + 1))

    def turn(axis, g, i):
        first, count = groups[g]
        some = pl.ds(first, count)
        if axis == 0:
            return remote(mid_a.at[some, i], recv_a.at[some, i], turn_sem, (0, g, i), in_column(i, 1))
        return remote(mid_b.at[some, i], recv_b.at[i, some], turn_sem, (1, g, i), in_row(i, 1))

    def in1_a(c, q):
        two = pl.ds(2 * c, 2)
        return remote(outs_a.at[two, q], back_a.at[two, q], cross_sem, (0, c, q), in_column(q, -1))

    def in1_b(p):
        return remote(outs_b.at[p], back_b.at[p], line_sem, (0, p), in_row(p, -1))

    back, gath, part, land = (back_a, back_b), (gath_a, gath_b), (part_a, part_b), (land_a, land_b)
    wide = (cut, tokens_ref.shape[1] - cut)

    def piece(axis, h):
        return pl.ds(h * (wide[axis] // 2), wide[axis] // 2)

    def gather(axis, way, b, n):
        at = (axis, way, b, n)
        target = step(axis, way, -(b + 1))
        i = far if b == 2 else 2 + 2 * b + way
        low = pl.ds(way * half, half) if b == 2 else pl.ds(0, side)
        into = pl.ds(b * side, half if b == 2 else side)
        if axis == 0:
            lanes = piece(0, n)
            return remote(back_a.at[i, low, :, lanes], gath_a.at[way, into, :, lanes], gath_sem, at, target)
        lanes = pl.ds(0, wide[1]) if n == 2 else piece(1, n)
        if b < 2:
            first = 0 if n == 2 else half
            low, into = pl.ds(first, half), pl.ds(b * side + first, half)
        return remote(back_b.at[low, i, :, lanes], gath_b.at[way, into, :, lanes], gath_sem, at, target)

    early_b = [(way, b, 2) for b in range(3) for way in range(2) if b < 2 or way == 0]

    def late_b(n):
        return [(way, b, n) for b in range(3) for way in range(2) if b < 2 or way == 1]

    def whole_a(n):
        return [(way, b, n) for b in range(3) for way in range(2)]

    def hand(axis, way, h):
        lanes = piece(axis, h)
        return remote(
            part[axis].at[way, :, lanes],
            land[axis].at[way, :, lanes],
            part_sem,
            (axis, way, h),
            step(axis, way, -1),
        )

    barrier = pltpu.get_barrier_semaphore()

    @pl.loop(1, side)
    def _(d):
        pl.semaphore_signal(barrier, inc=1, device_id={"ep": at_column(d)}, device_id_type=MESH)
        pl.semaphore_signal(barrier, inc=1, device_id={"ep": at_row(d)}, device_id_type=MESH)

    pl.semaphore_signal(barrier, inc=1, device_id={"tp": 1 - tp}, device_id_type=MESH)

    local = [
        pltpu.make_async_copy(src.at[0], dst.at[tp], local_sem.at[i])
        for i, (src, dst) in enumerate(((wg_hbm, wg), (wu_hbm, wu), (wd_hbm, wd)))
    ]
    for copy in local:
        copy.start()

    values = tokens_ref[...].astype(F32)
    scale = lax.rsqrt(jnp.mean(values * values, axis=-1, keepdims=True) + 1e-06)
    whole = (values * scale * gain_ref[...]).astype(BF16)
    normed_a[...] = whole[:, :cut]
    normed_b[...] = whole[:, cut:]

    pl.semaphore_wait(barrier, 2 * side - 1)
    for axis in range(2):
        for way in range(2):
            give(axis, way).start()

    ids = ids_ref[...]
    gates = gates_ref[...]
    below = lax.broadcasted_iota(jnp.int32, (n_ep, n_tok), 0)
    hots = [(ids[k : k + 1] == below).astype(F32) for k in range(ids.shape[0])]
    earlier = (
        lax.broadcasted_iota(jnp.int32, (n_tok, n_tok), 0)
        < lax.broadcasted_iota(jnp.int32, (n_tok, n_tok), 1)
    ).astype(BF16)
    before = jnp.dot(sum(hots).astype(BF16), earlier, preferred_element_type=F32)

    slots = []
    info[...] = jnp.zeros_like(info)
    for k, hot in enumerate(hots):
        e = ids[k : k + 1]
        nth = jnp.sum(before * hot, axis=0, keepdims=True).astype(jnp.int32)
        q = place((e // side - my + side) % side)
        p = place((e % side - mx + side) % side)
        slots.append((p * side + q) * cap + nth)
        info[k : k + 1] = slots[k].astype(F32)
        info[len(hots) + k : len(hots) + k + 1] = gates[k : k + 1]
    for axis in range(2):
        for way in range(2):
            tell(axis, way).start()

    def slot_of(axis, at, r):
        return at * line + r if axis == 0 else r // cap * line + at * cap + r % cap

    def choose(names, wanted, value):
        hit = sum((name == wanted).astype(F32) for name in names).astype(BF16)
        return jnp.dot(hit, value, preferred_element_type=F32).astype(BF16)

    def weigh_into(ref, names, wanted, shares):
        high = [g.astype(BF16).astype(F32) for g in shares]
        for n, split in enumerate((high, [g - h for g, h in zip(shares, high)])):
            ref[n] = sum(jnp.where(name == wanted, g, 0.0) for name, g in zip(names, split)).astype(BF16)

    def mix(ref, rows_of, value):
        return sum(
            lax.dot_general(ref[n, rows_of], value, (((0,), (0,)), ((), ())), preferred_element_type=F32)
            for n in range(2)
        )

    r = lax.broadcasted_iota(jnp.int32, (line, n_tok), 0)
    for axis in range(2):
        weigh_into(weigh_own.at[axis], slots, slot_of(axis, own, r), [gates[k : k + 1] for k in range(len(slots))])
        mine = choose(slots, slot_of(axis, own, r), normed[axis][...])
        mid[axis][own] = mine.reshape(side, cap, -1)

    def turn_group(g):
        def do(i):
            turn(0, g, i).start()
            turn(1, g, i).start()

        others(do)

    turn_group(pairs - 1)

    for copy in local:
        copy.wait()
    swaps = [
        pltpu.make_async_remote_copy(
            src_ref=ref.at[tp],
            dst_ref=ref.at[tp],
            send_sem=swap_sem.at[0, i],
            recv_sem=swap_sem.at[1, i],
            device_id={"tp": 1 - tp},
            device_id_type=MESH,
        )
        for i, ref in enumerate((wg, wu, wd))
    ]
    for swap in swaps:
        swap.start()

    r = lax.broadcasted_iota(jnp.int32, (3 * line + line // 2, n_tok), 0)
    for way in range(2):
        for axis in range(2):
            b = r // line
            inner = r % line + jnp.where(b == 3, way * (line // 2), 0)
            wanted = slot_of(axis, jnp.where(b == 3, far, 2 * b + way), inner)
            tell(axis, way).wait_recv()
            names = [infos[axis, way, k : k + 1].astype(jnp.int32) for k in range(len(slots))]
            give(axis, way).wait_recv()
            chosen = choose(names, wanted, tok[axis][way])
            mid[axis][way] = chosen[:line].reshape(side, cap, -1)
            stage[axis][way] = chosen[line:].reshape(2 * side + half, cap, -1)
            for b in range(3):
                relay(axis, way, b).start()
            shares = [infos[axis, way, len(slots) + k : len(slots) + k + 1] for k in range(len(slots))]
            weigh_into(weigh.at[axis, way], names, wanted, shares)

    turn_group(0)
    for b in range(3):
        for axis in range(2):
            for way in range(2):
                relay(axis, way, b).wait_recv()
        if b == 0:
            turn_group(1)

    def last_turns(i):
        for g in (2, pairs):
            turn(0, g, i).start()
            turn(1, g, i).start()

    others(last_turns)

    recv_a[:, own] = mid_a[:, own]
    recv_b[own] = mid_b[:, own]
    for swap in swaps:
        swap.wait()

    for c in range(pairs):
        for g in ((c,) if c < pairs - 1 else (c, c + 1)):
            others(lambda q: turn(0, g, q).wait_recv())
        for p in (2 * c, 2 * c + 1):
            if p != own:
                for g in range(len(groups)):
                    turn(1, g, p).wait_recv()

        two = pl.ds(2 * c, 2)
        taken_a = recv_a[two].reshape(rows, -1)
        taken_b = recv_b[two].reshape(rows, -1)
        total = None
        for j in range(wg.shape[0]):
            gate_act, up_act = (
                jnp.dot(taken_a, w[j, :cut], preferred_element_type=F32)
                + jnp.dot(taken_b, w[j, cut:], preferred_element_type=F32)
                for w in (wg, wu)
            )
            hidden = (gate_act / (1.0 + jnp.exp(-gate_act)) * up_act).astype(BF16)
            partial = jnp.dot(hidden, wd[j], preferred_element_type=F32).astype(BF16).astype(F32)
            total = partial if total is None else total + partial
        total = total.astype(BF16)
        outs_a[two] = total[:, :cut].reshape(2, side, cap, cut)
        outs_b[two] = total[:, cut:].reshape(2, side, cap, -1)
        others(lambda q: in1_a(c, q).start())
        for p in (2 * c, 2 * c + 1):
            if p != own:
                in1_b(p).start()

    back_a[:, own] = outs_a[:, own]
    back_b[own] = outs_b[own]

    def send(axis, which):
        for way, b, n in which:
            gather(axis, way, b, n).start()

    for c in range(pairs):
        for p in (2 * c, 2 * c + 1):
            if p != own:
                in1_b(p).wait_recv()
        others(lambda q: in1_a(c, q).wait_recv())
        if c == 1:
            send(1, early_b)
        if c:
            send(0, [(way, c - 1, 0) for way in range(2)])
    send(1, late_b(0))
    send(0, whole_a(1))
    send(1, late_b(1))

    def kept(axis, i, lanes):
        value = back_a[i, :, :, lanes] if axis == 0 else back_b[:, i, :, lanes]
        return value.reshape(line, -1)

    for h in range(2):
        for axis in range(2):
            lanes = piece(axis, h)
            for way in range(2):
                for w, b, n in (whole_a(h), late_b(h) + (early_b if h == 0 else []))[axis]:
                    if w == way:
                        gather(axis, way, b, n).wait_recv()
                got = mix(weigh.at[axis, way], pl.ds(0, line), kept(axis, way, lanes))
                got += mix(
                    weigh.at[axis, way],
                    pl.ds(line, 2 * line + line // 2),
                    gath[axis][way, :, :, lanes].reshape(2 * line + line // 2, -1),
                )
                part[axis][way, :, lanes] = got.astype(BF16)
                hand(axis, way, h).start()

    for h in range(2):
        for axis in range(2):
            lanes = piece(axis, h)
            got = mix(weigh_own.at[axis], pl.ds(0, line), kept(axis, own, lanes))
            for way in range(2):
                hand(axis, way, h).wait_recv()
                got += land[axis][way, :, lanes].astype(F32)
            out_ref[:, pl.ds(axis * cut + h * (wide[axis] // 2), wide[axis] // 2)] = got.astype(out_ref.dtype)

    for way, b, n in whole_a(0) + whole_a(1):
        gather(0, way, b, n).wait_send()
    for way, b, n in early_b + late_b(0) + late_b(1):
        gather(1, way, b, n).wait_send()
    for axis in range(2):
        for way in range(2):
            tell(axis, way).wait_send()
            give(axis, way).wait_send()
            for h in range(2):
                hand(axis, way, h).wait_send()
            for b in range(3):
                relay(axis, way, b).wait_send()

    def drain(i):
        in1_b(i).wait_send()
        for g in range(len(groups)):
            turn(0, g, i).wait_send()
            turn(1, g, i).wait_send()
        for c in range(pairs):
            in1_a(c, i).wait_send()

    others(drain)


def shards(n_ep, n_tp, tokens, norm_gain, expert_ids, gate_weights, w_gate, w_up, w_down):
    n_tok, width = tokens.shape
    top_count = expert_ids.shape[1]
    n_exp = w_gate.shape[0] * n_ep
    side = math.isqrt(n_ep)
    cap = top_count * (n_tok // 2) // (n_exp // N_GROUPS)
    cut = width // 2
    rows = 2 * side * cap
    hidden = w_gate.shape[2]
    vmem = pl.BlockSpec(memory_space=pltpu.VMEM)
    anywhere = pl.BlockSpec(memory_space=pl.ANY)
    dma = pltpu.SemaphoreType.DMA
    part_a = pltpu.VMEM((side, side, cap, cut), BF16)
    part_b = pltpu.VMEM((side, side, cap, width - cut), BF16)
    mixed = pl.pallas_call(
        functools.partial(kernel, side, cap, cut),
        out_shape=jax.ShapeDtypeStruct((n_tok, width), BF16),
        in_specs=[vmem] * 4 + [anywhere] * 3,
        out_specs=vmem,
        scratch_shapes=[
            pltpu.VMEM((8, n_tok), F32),
            pltpu.VMEM((2, 2, 8, n_tok), F32),
            pltpu.VMEM((2, 2, 2, 7 * side * cap // 2, n_tok), BF16),
            pltpu.VMEM((2, 2, side * cap, n_tok), BF16),
            pltpu.VMEM((n_tok, cut), BF16),
            pltpu.VMEM((n_tok, width - cut), BF16),
            pltpu.VMEM((2, n_tok, cut), BF16),
            pltpu.VMEM((2, n_tok, width - cut), BF16),
            pltpu.VMEM((2, 2 * side + side // 2, cap, cut), BF16),
            pltpu.VMEM((2, 2 * side + side // 2, cap, width - cut), BF16),
            *([part_a, part_b] * 4),
            pltpu.VMEM((2, 2 * side + side // 2, cap, cut), BF16),
            pltpu.VMEM((2, 2 * side + side // 2, cap, width - cut), BF16),
            *([pltpu.VMEM((2, n_tok, cut), BF16), pltpu.VMEM((2, n_tok, width - cut), BF16)] * 2),
            pltpu.VMEM((n_tp, width, hidden), BF16),
            pltpu.VMEM((n_tp, width, hidden), BF16),
            pltpu.VMEM((n_tp, hidden, width), BF16),
            dma((3,)),
            dma((2, 3)),
            dma((2, 2, 2)),
            dma((2, 2, 2)),
            dma((2, 2, 2, 3)),
            dma((2, 2, side // 2 + 1, side)),
            dma((2, 1, side)),
            dma((2, 1, side // 2, side)),
            dma((2, 2, 2, 3, 3)),
            dma((2, 2, 2, 2)),
        ],
        compiler_params=pltpu.CompilerParams(
            collective_id=0, has_side_effects=True, vmem_limit_bytes=60 * 1024 * 1024
        ),
    )(tokens, norm_gain.reshape(1, width), expert_ids.T, gate_weights.T, w_gate, w_up, w_down)
    return mixed


def solution(mesh):
    placed = (
        P(("grp", "ep", "tp"), None),
        P(),
        P(("grp", "ep", "tp"), None),
        P(("grp", "ep", "tp"), None),
        P("ep", None, "tp"),
        P("ep", None, "tp"),
        P("ep", "tp", None),
    )
    return jax.shard_map(
        functools.partial(shards, mesh.shape["ep"], mesh.shape["tp"]),
        mesh=mesh,
        in_specs=placed,
        out_specs=P(("grp", "ep", "tp"), None),
        check_vma=False,
    )
```

```python
import functools
import math

import jax
import jax.numpy as jnp
from jax import lax
from jax.experimental import pallas as pl
from jax.experimental.pallas import tpu as pltpu
from jax.sharding import PartitionSpec as P

N_GROUPS = 4
MESH = pl.DeviceIdType.MESH
BF16 = jnp.bfloat16
F32 = jnp.float32


def kernel(
    side,
    cap,
    cut,
    tokens_ref,
    gain_ref,
    ids_ref,
    gates_ref,
    wg_hbm,
    wu_hbm,
    wd_hbm,
    out_ref,
    info,
    infos,
    weigh,
    weigh_own,
    normed_a,
    normed_b,
    tok_a,
    tok_b,
    stage_a,
    stage_b,
    mid_a,
    mid_b,
    recv_a,
    recv_b,
    outs_a,
    outs_b,
    back_a,
    back_b,
    gath_a,
    gath_b,
    part_a,
    part_b,
    land_a,
    land_b,
    wg,
    wu,
    wd,
    local_sem,
    swap_sem,
    info_sem,
    tok_sem,
    relay_sem,
    turn_sem,
    line_sem,
    cross_sem,
    gath_sem,
    part_sem,
    word_sem,
):
    n_ep = side * side
    half = side // 2
    pairs = half
    own, far = side - 2, side - 1
    ep = lax.axis_index("ep")
    tp = lax.axis_index("tp")
    my, mx = ep // side, lax.rem(ep, side)
    n_tok = tokens_ref.shape[0]
    line = side * cap
    rows = 2 * line
    groups = [(2 * c, 2) for c in range(pairs - 1)] + [(own, 1), (far, 1)]

    def shift(p):
        k = p // 2
        return jnp.where(k == half - 1, p % 2 * half, jnp.where(p % 2 == 0, k + 1, side - 1 - k))

    def place(d):
        near = jnp.where(d < half, 2 * (d - 1), 2 * (side - d) - 1)
        return jnp.where(d == 0, own, jnp.where(d == half, far, near))

    def at_column(d):
        return my * side + lax.rem(mx + d + side, side)

    def at_row(d):
        return lax.rem(my + d + side, side) * side + mx

    def in_row(p, sign):
        return at_column(sign * shift(p))

    def in_column(q, sign):
        return at_row(sign * shift(q))

    def others(do):
        @pl.loop(0, side - 1)
        def _(i):
            do(jnp.where(i == own, far, i))

    def remote(src, dst, sems, at, target):
        return pltpu.make_async_remote_copy(
            src_ref=src,
            dst_ref=dst,
            send_sem=sems.at[(0, *at)],
            recv_sem=sems.at[(1, *at)],
            device_id={"ep": target},
            device_id_type=MESH,
        )

    def step(axis, way, far_by):
        return (at_column, at_row)[axis](far_by * (1 - 2 * way))

    normed = (normed_a, normed_b)
    tok, stage, mid = (tok_a, tok_b), (stage_a, stage_b), (mid_a, mid_b)

    def tell(axis, way):
        return remote(info, infos.at[axis, way], info_sem, (axis, way), step(axis, way, 1))

    def give(axis, way):
        return remote(normed[axis], tok[axis].at[way], tok_sem, (axis, way), step(axis, way, 1))

    def relay(axis, way, b):
        at = (axis, way, b)
        if b < 2:
            src, dst = stage[axis].at[way, pl.ds(b * side, side)], mid[axis].at[2 + 2 * b + way]
        else:
            src = stage[axis].at[way, pl.ds(2 * side, half)]
            dst = mid[axis].at[far, pl.ds(way * half, half)]
        return remote(src, dst, relay_sem, at, step(axis, way, b + 1))

    def turn(axis, g, i):
        first, count = groups[g]
        some = pl.ds(first, count)
        if axis == 0:
            return remote(mid_a.at[some, i], recv_a.at[some, i], turn_sem, (0, g, i), in_column(i, 1))
        return remote(mid_b.at[some, i], recv_b.at[i, some], turn_sem, (1, g, i), in_row(i, 1))

    def in1_a(c, q):
        two = pl.ds(2 * c, 2)
        return remote(outs_a.at[two, q], back_a.at[two, q], cross_sem, (0, c, q), in_column(q, -1))

    def in1_b(p):
        return remote(outs_b.at[p], back_b.at[p], line_sem, (0, p), in_row(p, -1))

    back, gath, part, land = (back_a, back_b), (gath_a, gath_b), (part_a, part_b), (land_a, land_b)
    wide = (cut, tokens_ref.shape[1] - cut)

    def piece(axis, h):
        return pl.ds(h * (wide[axis] // 2), wide[axis] // 2)

    def gather(axis, way, b, n):
        at = (axis, way, b, n)
        target = step(axis, way, -(b + 1))
        i = far if b == 2 else 2 + 2 * b + way
        low = pl.ds(way * half, half) if b == 2 else pl.ds(0, side)
        into = pl.ds(b * side, half if b == 2 else side)
        if axis == 0:
            lanes = piece(0, n)
            return remote(back_a.at[i, low, :, lanes], gath_a.at[way, into, :, lanes], gath_sem, at, target)
        lanes = pl.ds(0, wide[1]) if n == 2 else piece(1, n)
        if b < 2:
            first = 0 if n == 2 else half
            low, into = pl.ds(first, half), pl.ds(b * side + first, half)
        return remote(back_b.at[low, i, :, lanes], gath_b.at[way, into, :, lanes], gath_sem, at, target)

    early_b = [(way, b, 2) for b in range(3) for way in range(2) if b < 2 or way == 0]

    def late_b(n):
        return [(way, b, n) for b in range(3) for way in range(2) if b < 2 or way == 1]

    def whole_a(n):
        return [(way, b, n) for b in range(3) for way in range(2)]

    def hand(axis, way, h):
        lanes = piece(axis, h)
        return remote(
            part[axis].at[way, :, lanes],
            land[axis].at[way, :, lanes],
            part_sem,
            (axis, way, h),
            step(axis, way, -1),
        )

    barrier = pltpu.get_barrier_semaphore()

    for axis in range(2):
        for way in range(2):
            pl.semaphore_signal(barrier, inc=1, device_id={"ep": step(axis, way, 1)}, device_id_type=MESH)

    pl.semaphore_signal(barrier, inc=1, device_id={"tp": 1 - tp}, device_id_type=MESH)

    local = [
        pltpu.make_async_copy(src.at[0], dst.at[tp], local_sem.at[i])
        for i, (src, dst) in enumerate(((wg_hbm, wg), (wu_hbm, wu), (wd_hbm, wd)))
    ]
    for copy in local:
        copy.start()

    values = tokens_ref[...].astype(F32)
    scale = lax.rsqrt(jnp.mean(values * values, axis=-1, keepdims=True) + 1e-06)
    whole = (values * scale * gain_ref[...]).astype(BF16)
    normed_a[...] = whole[:, :cut]
    normed_b[...] = whole[:, cut:]

    def pass_word(k):
        for axis in range(2):
            for way in range(2):
                if k:
                    pl.semaphore_wait(word_sem.at[k - 1, axis, way], 1)
                if k < half - 1:
                    pl.semaphore_signal(
                        word_sem.at[k, axis, way],
                        inc=1,
                        device_id={"ep": step(axis, way, 1)},
                        device_id_type=MESH,
                    )

    pl.semaphore_wait(barrier, 5)
    pass_word(0)
    for axis in range(2):
        for way in range(2):
            give(axis, way).start()

    ids = ids_ref[...]
    gates = gates_ref[...]
    pass_word(1)
    below = lax.broadcasted_iota(jnp.int32, (n_ep, n_tok), 0)
    hots = [(ids[k : k + 1] == below).astype(F32) for k in range(ids.shape[0])]
    earlier = (
        lax.broadcasted_iota(jnp.int32, (n_tok, n_tok), 0)
        < lax.broadcasted_iota(jnp.int32, (n_tok, n_tok), 1)
    ).astype(BF16)
    before = jnp.dot(sum(hots).astype(BF16), earlier, preferred_element_type=F32)

    slots = []
    info[...] = jnp.zeros_like(info)
    for k, hot in enumerate(hots):
        e = ids[k : k + 1]
        nth = jnp.sum(before * hot, axis=0, keepdims=True).astype(jnp.int32)
        q = place((e // side - my + side) % side)
        p = place((e % side - mx + side) % side)
        slots.append((p * side + q) * cap + nth)
        info[k : k + 1] = slots[k].astype(F32)
        info[len(hots) + k : len(hots) + k + 1] = gates[k : k + 1]
    for axis in range(2):
        for way in range(2):
            tell(axis, way).start()
    pass_word(2)

    def slot_of(axis, at, r):
        return at * line + r if axis == 0 else r // cap * line + at * cap + r % cap

    def choose(names, wanted, value):
        hit = sum((name == wanted).astype(F32) for name in names).astype(BF16)
        return jnp.dot(hit, value, preferred_element_type=F32).astype(BF16)

    def weigh_into(ref, names, wanted, shares):
        high = [g.astype(BF16).astype(F32) for g in shares]
        for n, split in enumerate((high, [g - h for g, h in zip(shares, high)])):
            ref[n] = sum(jnp.where(name == wanted, g, 0.0) for name, g in zip(names, split)).astype(BF16)

    def mix(ref, rows_of, value):
        return sum(
            lax.dot_general(ref[n, rows_of], value, (((0,), (0,)), ((), ())), preferred_element_type=F32)
            for n in range(2)
        )

    r = lax.broadcasted_iota(jnp.int32, (line, n_tok), 0)
    for axis in range(2):
        weigh_into(weigh_own.at[axis], slots, slot_of(axis, own, r), [gates[k : k + 1] for k in range(len(slots))])
        mine = choose(slots, slot_of(axis, own, r), normed[axis][...])
        mid[axis][own] = mine.reshape(side, cap, -1)

    def turn_group(g):
        def do(i):
            turn(0, g, i).start()
            turn(1, g, i).start()

        others(do)

    pass_word(3)
    turn_group(pairs - 1)

    for copy in local:
        copy.wait()
    swaps = [
        pltpu.make_async_remote_copy(
            src_ref=ref.at[tp],
            dst_ref=ref.at[tp],
            send_sem=swap_sem.at[0, i],
            recv_sem=swap_sem.at[1, i],
            device_id={"tp": 1 - tp},
            device_id_type=MESH,
        )
        for i, ref in enumerate((wg, wu, wd))
    ]
    for swap in swaps:
        swap.start()

    r = lax.broadcasted_iota(jnp.int32, (3 * line + line // 2, n_tok), 0)
    for way in range(2):
        for axis in range(2):
            b = r // line
            inner = r % line + jnp.where(b == 3, way * (line // 2), 0)
            wanted = slot_of(axis, jnp.where(b == 3, far, 2 * b + way), inner)
            tell(axis, way).wait_recv()
            names = [infos[axis, way, k : k + 1].astype(jnp.int32) for k in range(len(slots))]
            give(axis, way).wait_recv()
            chosen = choose(names, wanted, tok[axis][way])
            mid[axis][way] = chosen[:line].reshape(side, cap, -1)
            stage[axis][way] = chosen[line:].reshape(2 * side + half, cap, -1)
            for b in range(3):
                relay(axis, way, b).start()
            shares = [infos[axis, way, len(slots) + k : len(slots) + k + 1] for k in range(len(slots))]
            weigh_into(weigh.at[axis, way], names, wanted, shares)

    turn_group(0)
    for b in range(3):
        for axis in range(2):
            for way in range(2):
                relay(axis, way, b).wait_recv()
        if b == 0:
            turn_group(1)

    def last_turns(i):
        for g in (2, pairs):
            turn(0, g, i).start()
            turn(1, g, i).start()

    others(last_turns)

    recv_a[:, own] = mid_a[:, own]
    recv_b[own] = mid_b[:, own]
    for swap in swaps:
        swap.wait()

    for c in range(pairs):
        for g in ((c,) if c < pairs - 1 else (c, c + 1)):
            others(lambda q: turn(0, g, q).wait_recv())
        for p in (2 * c, 2 * c + 1):
            if p != own:
                for g in range(len(groups)):
                    turn(1, g, p).wait_recv()

        two = pl.ds(2 * c, 2)
        taken_a = recv_a[two].reshape(rows, -1)
        taken_b = recv_b[two].reshape(rows, -1)
        total = None
        for j in range(wg.shape[0]):
            gate_act, up_act = (
                jnp.dot(taken_a, w[j, :cut], preferred_element_type=F32)
                + jnp.dot(taken_b, w[j, cut:], preferred_element_type=F32)
                for w in (wg, wu)
            )
            hidden = (gate_act / (1.0 + jnp.exp(-gate_act)) * up_act).astype(BF16)
            partial = jnp.dot(hidden, wd[j], preferred_element_type=F32).astype(BF16).astype(F32)
            total = partial if total is None else total + partial
        total = total.astype(BF16)
        outs_a[two] = total[:, :cut].reshape(2, side, cap, cut)
        outs_b[two] = total[:, cut:].reshape(2, side, cap, -1)
        others(lambda q: in1_a(c, q).start())
        for p in (2 * c, 2 * c + 1):
            if p != own:
                in1_b(p).start()

    back_a[:, own] = outs_a[:, own]
    back_b[own] = outs_b[own]

    for axis in range(2):
        for way in range(2):
            tell(axis, way).wait_send()
            give(axis, way).wait_send()
            for b in range(3):
                relay(axis, way, b).wait_send()

    def drain(i):
        for g in range(len(groups)):
            turn(0, g, i).wait_send()
            turn(1, g, i).wait_send()

    others(drain)

    def send(axis, which):
        for way, b, n in which:
            gather(axis, way, b, n).start()

    for c in range(pairs):
        for p in (2 * c, 2 * c + 1):
            if p != own:
                in1_b(p).wait_recv()
        others(lambda q: in1_a(c, q).wait_recv())
        if c == 1:
            send(1, early_b)
        if c:
            send(0, [(way, c - 1, 0) for way in range(2)])
    send(1, late_b(0))
    send(0, whole_a(1))
    send(1, late_b(1))

    def drain_in1(i):
        in1_b(i).wait_send()
        for c in range(pairs):
            in1_a(c, i).wait_send()

    others(drain_in1)

    def kept(axis, i, lanes):
        value = back_a[i, :, :, lanes] if axis == 0 else back_b[:, i, :, lanes]
        return value.reshape(line, -1)

    for h in range(2):
        for axis in range(2):
            lanes = piece(axis, h)
            for way in range(2):
                for w, b, n in (whole_a(h), late_b(h) + (early_b if h == 0 else []))[axis]:
                    if w == way:
                        gather(axis, way, b, n).wait_recv()
                got = mix(weigh.at[axis, way], pl.ds(0, line), kept(axis, way, lanes))
                got += mix(
                    weigh.at[axis, way],
                    pl.ds(line, 2 * line + line // 2),
                    gath[axis][way, :, :, lanes].reshape(2 * line + line // 2, -1),
                )
                part[axis][way, :, lanes] = got.astype(BF16)
                hand(axis, way, h).start()

    for way, b, n in whole_a(0) + whole_a(1):
        gather(0, way, b, n).wait_send()
    for way, b, n in early_b + late_b(0) + late_b(1):
        gather(1, way, b, n).wait_send()

    for h in range(2):
        for axis in range(2):
            lanes = piece(axis, h)
            got = mix(weigh_own.at[axis], pl.ds(0, line), kept(axis, own, lanes))
            for way in range(2):
                hand(axis, way, h).wait_recv()
                got += land[axis][way, :, lanes].astype(F32)
            out_ref[:, pl.ds(axis * cut + h * (wide[axis] // 2), wide[axis] // 2)] = got.astype(out_ref.dtype)

    for axis in range(2):
        for way in range(2):
            for h in range(2):
                hand(axis, way, h).wait_send()


def shards(n_ep, n_tp, tokens, norm_gain, expert_ids, gate_weights, w_gate, w_up, w_down):
    n_tok, width = tokens.shape
    top_count = expert_ids.shape[1]
    n_exp = w_gate.shape[0] * n_ep
    side = math.isqrt(n_ep)
    cap = top_count * (n_tok // 2) // (n_exp // N_GROUPS)
    cut = width // 2
    rows = 2 * side * cap
    hidden = w_gate.shape[2]
    vmem = pl.BlockSpec(memory_space=pltpu.VMEM)
    anywhere = pl.BlockSpec(memory_space=pl.ANY)
    dma = pltpu.SemaphoreType.DMA
    part_a = pltpu.VMEM((side, side, cap, cut), BF16)
    part_b = pltpu.VMEM((side, side, cap, width - cut), BF16)
    mixed = pl.pallas_call(
        functools.partial(kernel, side, cap, cut),
        out_shape=jax.ShapeDtypeStruct((n_tok, width), BF16),
        in_specs=[vmem] * 4 + [anywhere] * 3,
        out_specs=vmem,
        scratch_shapes=[
            pltpu.VMEM((8, n_tok), F32),
            pltpu.VMEM((2, 2, 8, n_tok), F32),
            pltpu.VMEM((2, 2, 2, 7 * side * cap // 2, n_tok), BF16),
            pltpu.VMEM((2, 2, side * cap, n_tok), BF16),
            pltpu.VMEM((n_tok, cut), BF16),
            pltpu.VMEM((n_tok, width - cut), BF16),
            pltpu.VMEM((2, n_tok, cut), BF16),
            pltpu.VMEM((2, n_tok, width - cut), BF16),
            pltpu.VMEM((2, 2 * side + side // 2, cap, cut), BF16),
            pltpu.VMEM((2, 2 * side + side // 2, cap, width - cut), BF16),
            *([part_a, part_b] * 4),
            pltpu.VMEM((2, 2 * side + side // 2, cap, cut), BF16),
            pltpu.VMEM((2, 2 * side + side // 2, cap, width - cut), BF16),
            *([pltpu.VMEM((2, n_tok, cut), BF16), pltpu.VMEM((2, n_tok, width - cut), BF16)] * 2),
            pltpu.VMEM((n_tp, width, hidden), BF16),
            pltpu.VMEM((n_tp, width, hidden), BF16),
            pltpu.VMEM((n_tp, hidden, width), BF16),
            dma((3,)),
            dma((2, 3)),
            dma((2, 2, 2)),
            dma((2, 2, 2)),
            dma((2, 2, 2, 3)),
            dma((2, 2, side // 2 + 1, side)),
            dma((2, 1, side)),
            dma((2, 1, side // 2, side)),
            dma((2, 2, 2, 3, 3)),
            dma((2, 2, 2, 2)),
            pltpu.SemaphoreType.REGULAR((side // 2 - 1, 2, 2)),
        ],
        compiler_params=pltpu.CompilerParams(
            collective_id=0, has_side_effects=True, vmem_limit_bytes=60 * 1024 * 1024
        ),
    )(tokens, norm_gain.reshape(1, width), expert_ids.T, gate_weights.T, w_gate, w_up, w_down)
    return mixed


def solution(mesh):
    placed = (
        P(("grp", "ep", "tp"), None),
        P(),
        P(("grp", "ep", "tp"), None),
        P(("grp", "ep", "tp"), None),
        P("ep", None, "tp"),
        P("ep", None, "tp"),
        P("ep", "tp", None),
    )
    return jax.shard_map(
        functools.partial(shards, mesh.shape["ep"], mesh.shape["tp"]),
        mesh=mesh,
        in_specs=placed,
        out_specs=P(("grp", "ep", "tp"), None),
        check_vma=False,
    )
```
